32 devices in a mesh: ep: 8 (over z, x), tp: 4 (over y, core).
Axes of the slice: x: 2, y: 2, z: 4, core: 2. Of those that a mesh axis runs over, the one named last changes fastest.
Arguments:
- conv_value: bfloat16 [4096, 2048], P('ep', 'tp'), may hold values from -6 to 6
- conv_gate: bfloat16 [4096, 2048], P('ep', 'tp'), may hold values from -9 to 9
- conv_taps: float32 [31, 2048], P(None, 'tp'), may hold values from -14 to 14
- norm_gain: float32 [2048], P('tp'), may hold values from 0.1 to 1.9
- norm_shift: float32 [2048], P('tp'), may hold values from -3 to 3
- conv_out_weight: bfloat16 [2048, 2048], P(None, 'tp'), may hold values from -0.125 to 0.125
- moe_input: bfloat16 [1024, 2048], P('ep'), may hold values from -6 to 6
- moe_gain: float32 [2048], replicated, may hold values from 0.1 to 1.9
- routes: int32 [1024, 4], P('ep'), may hold values from 0 to 7, all different within a row; in each aligned block of 128 rows (0 to 127, 128 to 255, ...) at most 128 rows name the same one
- route_weights: float32 [1024, 4], P('ep'), may hold values from 0.25 to 1
- expert_gate: bfloat16 [8, 2048, 4096], P('ep', None, 'tp'), may hold values from -0.125 to 0.125
- expert_up: bfloat16 [8, 2048, 4096], P('ep', None, 'tp'), may hold values from -0.125 to 0.125
- expert_down: bfloat16 [8, 4096, 2048], P('ep', None, 'tp'), may hold values from -0.09375 to 0.09375
- shared_gate: bfloat16 [2048, 512], P(None, 'tp'), may hold values from -0.125 to 0.125
- shared_up: bfloat16 [2048, 512], P(None, 'tp'), may hold values from -0.125 to 0.125
- shared_down: bfloat16 [512, 2048], P(None, 'tp'), may hold values from -0.25 to 0.25
Outputs:
- conv_result: bfloat16 [4096, 2048], P('ep', 'tp')
- moe_result: bfloat16 [1024, 2048], P('ep', 'tp')
The draws below stay inside these ranges and needn't reach their ends.
Inputs may be any that keep to these rules, and one draw needn't show every extreme that they name: `routes`: in the rows of one device (aligned blocks of 128 rows) no expert is named by more than 128 rows, a bound that some block reaches; each row names 4 different experts.
All inputs are finite; a program needn't handle non-finite values.
Results may differ from the reference program's by a relative error of at most 0.0068.
Values may be sent and summed in bfloat16 or wider, within the bound.
No kernel may reach another device: no remote copies, remote signals or barrier semaphores. Data moves between devices by JAX's collectives and lax.ppermute only.
A program may use at most 64 MiB of HBM per device.

```python
import math
import jax
import jax.numpy as jnp
import numpy as np
from jax import lax

D = 2048
FF = 4096
SHARED_FF = 512
CONV_WIDTH = 31
TOPK = 4
TOKB_DEV = 128
TOK_A = 4096
TOK_B = 1024
EXPERTS = 8
CAP = 128
N_EP = 8


def draw_conv_taps(key, part):
    base_key = jax.random.fold_in(key, 11)
    rough_key = jax.random.fold_in(key, 12)
    channel = jnp.arange(D, dtype=jnp.float32) / D
    base_draw = jnp.clip(jax.random.normal(base_key, (CONV_WIDTH, D), jnp.float32), -5.0, 5.0)
    channel_rise = jnp.exp(jnp.log(4.0) * channel)
    rough_scale = jax.random.uniform(rough_key, (D,), jnp.float32, 0.5, 1.5)
    return base_draw * channel_rise * rough_scale / jnp.sqrt(CONV_WIDTH * 1.0)


def block_scale(stream_key, shape, split, least, high):
    factor_of = 1.0
    for dim, blocks in split:
        draws = jax.random.uniform(jax.random.fold_in(jax.random.fold_in(stream_key, 6), dim), (blocks,), jnp.float32, least / len(split), high / len(split))
        factor_of = factor_of * jnp.repeat(jnp.exp(draws), shape[dim] // blocks).reshape((-1,) + (1,) * (len(shape) - 1 - dim))
    return factor_of


def routed_block(stream_key, own, number, rows, number_of, top, most, skew):
    order = jax.random.permutation(stream_key, number_of)
    packed, common = shares(number_of, rows * top, most, skew, True), shares(number_of, rows * top, most, skew, False)
    places = jnp.arange(number_of)

    def named(sizes, rotation):
        used = int((sizes > 0).sum())
        fixed = max(1, used // 4)
        shifted = fixed + (places - fixed + rotation * (used - fixed)) % max(1, number_of - fixed)
        return jnp.zeros((number_of,), jnp.int32).at[order[jnp.where(places < fixed, places, shifted)]].set(jnp.asarray(sizes, jnp.int32))

    sizes = jnp.where(number % 4 == 0, named(packed, number // 4), named(common, number - number // 4 - 1))
    mixed = jax.random.permutation(jax.random.fold_in(own, 3), number_of)
    giver, receiver = mixed[0:number_of // 2 * 2:2], mixed[1:number_of // 2 * 2:2]
    slack = jnp.minimum(sizes[giver] - 1, most - sizes[receiver]) // 2
    slack = jnp.where((giver == order[0]) | (receiver == order[0]) | (sizes[receiver] == 0), 0, jnp.maximum(slack, 0))
    shifted = jax.random.randint(jax.random.fold_in(own, 4), (number_of // 2,), 0, 1 << 20) % (slack + 1)
    sizes = sizes.at[giver].add(-shifted).at[receiver].add(shifted)
    items = jnp.searchsorted(jnp.cumsum(sizes), jnp.arange(rows * top), side="right").astype(jnp.int32)
    listing = items.reshape(top, rows).T
    listing = listing[jax.random.permutation(jax.random.fold_in(own, 1), rows)]
    rotation = jax.random.randint(jax.random.fold_in(own, 2), (rows, 1), 0, top)
    return jnp.take_along_axis(listing, (jnp.arange(top)[None, :] + rotation) % top, axis=1)


def shares(amount, total, reach, skew, full):
    portions = [(1 << 20) // math.isqrt(rank ** skew) + 1 for rank in range(1, amount + 1)]
    largest = reach if full else min(reach, max(-(-total // amount), total * portions[0] // sum(portions)))
    least = 1 if total - largest >= amount - 1 else 0
    given, surplus = [largest] + [least] * (amount - 1), total - largest - least * (amount - 1)
    while surplus > 0:
        movable = [i for i in range(1, amount) if given[i] < largest] or [i for i in range(1, amount) if given[i] < reach]
        whole, left = sum([portions[i] for i in movable]), surplus
        for i in movable:
            extra = min(reach - given[i], max(1, left * portions[i] // whole), surplus)
            given[i] = given[i] + extra
            surplus = surplus - extra
    return np.array(given)


def noise(rng, shape, width, reach, shards=(), kind=jnp.bfloat16):
    array = jax.random.normal(rng, shape, jnp.float32) * width
    if len(shards) > 0:
        array = block_scale(rng, shape, shards, -0.22, 0.18) * array
    return jnp.clip(array, min=-reach, max=reach).astype(kind)


def setup_inputs(seed: int = 0) -> dict:
    key_list = jax.random.split(jax.random.key(seed), 17)
    conv_value = noise(key_list[0], (TOK_A, D), 1.0, 6.0, ((0, 8), (1, 4)))
    conv_gate = noise(key_list[1], (TOK_A, D), 1.5, 9.0, ((0, 8), (1, 4)))
    conv_taps = draw_conv_taps(jax.random.fold_in(key_list[16], 71), 0)
    norm_gain = jnp.clip(1.0 + 0.18 * jax.random.normal(key_list[3], (D,), jnp.float32), 0.1, 1.9)
    norm_shift = noise(key_list[4], (D,), 0.5, 3.0, ((0, 4),), jnp.float32)
    conv_out_weight = noise(key_list[5], (D, D), D ** -0.5, 0.125, ((1, 4),))
    moe_input = noise(key_list[6], (TOK_B, D), 1.0, 6.0, ((0, 8),))
    moe_gain = jnp.clip(1.0 + 0.18 * jax.random.normal(key_list[7], (D,), jnp.float32), 0.1, 1.9)
    routes_keys = jax.random.split(jax.random.fold_in(key_list[8], 1), TOK_B // TOKB_DEV)
    routes_turns = jax.random.permutation(jax.random.fold_in(key_list[8], 3), TOK_B // TOKB_DEV)
    routes = jax.vmap(lambda own, number: routed_block(jax.random.fold_in(key_list[8], 2), own, number, TOKB_DEV, EXPERTS, TOPK, CAP, 2))(routes_keys, routes_turns).reshape((TOK_B, TOPK))
    route_weights = jnp.clip(0.25 + 0.75 * jax.random.uniform(key_list[9], (TOK_B, TOPK), jnp.float32) ** block_scale(key_list[9], (TOK_B, TOPK), ((0, 8),), -0.2, 0.2), 0.25, 1.0)
    expert_gate = noise(key_list[10], (EXPERTS, D, FF), D ** -0.5, 0.125, ((0, 8), (2, 4)))
    expert_up = noise(key_list[11], (EXPERTS, D, FF), D ** -0.5, 0.125, ((0, 8), (2, 4)))
    expert_down = noise(key_list[12], (EXPERTS, FF, D), FF ** -0.5, 0.09375, ((0, 8), (2, 4)))
    shared_gate = noise(key_list[13], (D, SHARED_FF), D ** -0.5, 0.125, ((1, 4),))
    shared_up = noise(key_list[14], (D, SHARED_FF), D ** -0.5, 0.125, ((1, 4),))
    shared_down = noise(key_list[15], (SHARED_FF, D), SHARED_FF ** -0.5, 0.25, ((1, 4),))
    return {"conv_value": conv_value, "conv_gate": conv_gate, "conv_taps": conv_taps, "norm_gain": norm_gain, "norm_shift": norm_shift, "conv_out_weight": conv_out_weight, "moe_input": moe_input, "moe_gain": moe_gain, "routes": routes, "route_weights": route_weights, "expert_gate": expert_gate, "expert_up": expert_up, "expert_down": expert_down, "shared_gate": shared_gate, "shared_up": shared_up, "shared_down": shared_down}


def reference(conv_value, conv_gate, conv_taps, norm_gain, norm_shift, conv_out_weight, moe_input, moe_gain, routes, route_weights, expert_gate, expert_up, expert_down, shared_gate, shared_up, shared_down):
    glu_rows = (conv_value.astype(jnp.float32) * jax.nn.sigmoid(conv_gate.astype(jnp.float32))).astype(jnp.bfloat16)
    padded = jnp.concatenate([jnp.zeros((CONV_WIDTH - 1, D), jnp.bfloat16), glu_rows], axis=0)
    filtered = jnp.zeros((TOK_A, D), jnp.float32)
    for offset in range(CONV_WIDTH):
        filtered = filtered + conv_taps[offset] * padded[offset:offset + TOK_A].astype(jnp.float32)
    row_mean = lax.optimization_barrier(jnp.mean(filtered, axis=1, keepdims=True))
    row_square = lax.optimization_barrier(jnp.mean(filtered * filtered, axis=1, keepdims=True))
    scaled = (filtered - row_mean) * lax.rsqrt(row_square - row_mean * row_mean + 1e-05)
    conv_hidden = jax.nn.silu(scaled * norm_gain + norm_shift).astype(jnp.bfloat16)
    conv_result = jnp.dot(conv_hidden, conv_out_weight, preferred_element_type=jnp.float32).astype(jnp.bfloat16)
    inputs = moe_input.astype(jnp.float32)
    normed = (inputs * lax.rsqrt(lax.optimization_barrier(jnp.mean(inputs * inputs, axis=1, keepdims=True)) + 1e-06) * moe_gain).astype(jnp.bfloat16)
    flat_expert = routes.reshape(-1).astype(jnp.int32)
    owner_row = (jnp.arange(TOK_B * TOPK, dtype=jnp.int32) // TOPK).astype(jnp.int32)
    sort_order = jnp.argsort(flat_expert, stable=True).astype(jnp.int32)
    sorted_owner = owner_row[sort_order]
    sorted_weight = route_weights.reshape(-1)[sort_order]
    counts = lax.optimization_barrier(jnp.sum((flat_expert[:, None] == jnp.arange(EXPERTS, dtype=jnp.int32)[None, :]).astype(jnp.int32), axis=0))
    starts = (jnp.cumsum(counts) - counts).astype(jnp.int32)
    slot_limit = N_EP * CAP
    pad_owner = jnp.concatenate([sorted_owner, jnp.zeros((slot_limit,), jnp.int32)])
    pad_weight = jnp.concatenate([sorted_weight, jnp.zeros((slot_limit,), jnp.float32)])

    def one_expert(running, expert_id):
        first_row = starts[expert_id]
        row_ids = lax.dynamic_slice_in_dim(pad_owner, first_row, slot_limit)
        weight = lax.dynamic_slice_in_dim(pad_weight, first_row, slot_limit)
        live_mask = (jnp.arange(slot_limit, dtype=jnp.int32) < counts[expert_id]).astype(jnp.float32)
        picked_rows = normed[row_ids]
        hidden = (jax.nn.silu(jnp.dot(picked_rows, expert_gate[expert_id], preferred_element_type=jnp.float32)) * jnp.dot(picked_rows, expert_up[expert_id], preferred_element_type=jnp.float32)).astype(jnp.bfloat16)
        expert_rows = jnp.dot(hidden, expert_down[expert_id], preferred_element_type=jnp.float32).astype(jnp.bfloat16)
        expert_rows = lax.optimization_barrier(expert_rows).astype(jnp.float32)
        return (running.at[row_ids].add(expert_rows * (weight * live_mask)[:, None]), None)
    routed, _ = lax.scan(one_expert, jnp.zeros((TOK_B, D), jnp.float32), jnp.arange(EXPERTS, dtype=jnp.int32))
    shared_hidden = (jax.nn.silu(jnp.dot(normed, shared_gate, preferred_element_type=jnp.float32)) * jnp.dot(normed, shared_up, preferred_element_type=jnp.float32)).astype(jnp.bfloat16)
    shared_sum = jnp.dot(shared_hidden, shared_down, preferred_element_type=jnp.float32)
    moe_result = (routed + shared_sum).astype(jnp.bfloat16)
    return (conv_result, moe_result)
```

```python
import jax
import jax.numpy as jnp
from jax import lax
from jax.sharding import PartitionSpec as P


PAIR = 2


def from_behind(value, axis, steps):
    count = lax.axis_size(axis)
    initial, last = (max(0, -steps), min(count, count - steps))
    return lax.ppermute(value, axis, [(source, source + steps) for source in range(initial, last)])


def moved(value, axis, steps, flip):
    count = lax.axis_size(axis)
    rings = count // PAIR
    return lax.ppermute(
        value,
        axis,
        [
            (source, ((source // PAIR + steps) % rings) * PAIR + (source % PAIR ^ flip))
            for source in range(count)
        ],
    )


def gathered(value):
    shares = [(value, moved(value, "tp", 0, 1))]
    for _ in range(lax.axis_size("tp") // PAIR - 1):
        value = moved(value, "tp", 1, 0)
        shares.append((value, moved(value, "tp", 0, 1)))
    return shares


def matching_rows(weight):
    count = lax.axis_size("tp")
    rings = count // PAIR
    index = lax.axis_index("tp")
    split = weight.reshape(count, weight.shape[0] // count, weight.shape[1])
    return [
        jnp.concatenate(
            [
                lax.dynamic_index_in_dim(
                    split, (index // PAIR + rings - back) % rings * PAIR + (index % PAIR ^ flip), 0, False
                )
                for flip in range(PAIR)
            ],
            axis=0,
        )
        for back in range(rings)
    ]


def contracted(shares, weights):
    total = None
    for pair, weight in zip(shares, weights):
        part = jnp.dot(
            jnp.concatenate(pair, axis=1), weight, preferred_element_type=jnp.float32
        )
        total = part if total is None else total + part
    return total


def summed(value):
    value = value + moved(value, "tp", 0, 1)
    total = value
    for _ in range(lax.axis_size("tp") // PAIR - 1):
        value = moved(value, "tp", 1, 0)
        total = total + value
    return total


def norm(moe_input, moe_gain):
    inputs = moe_input.astype(jnp.float32)
    return (
        inputs * lax.rsqrt(jnp.mean(inputs * inputs, axis=1, keepdims=True) + 1e-06) * moe_gain
    ).astype(jnp.bfloat16)


def gated(rows, gate, up):
    return (
        jax.nn.silu(jnp.dot(rows, gate, preferred_element_type=jnp.float32))
        * jnp.dot(rows, up, preferred_element_type=jnp.float32)
    ).astype(jnp.bfloat16)


def conv_module(conv_value, conv_gate, conv_taps, norm_gain, norm_shift, conv_out_weight):
    tap_count = conv_taps.shape[0]
    rows_a = conv_value.shape[0]
    glu_rows = (
        conv_value.astype(jnp.float32) * jax.nn.sigmoid(conv_gate.astype(jnp.float32))
    ).astype(jnp.bfloat16)
    before = from_behind(glu_rows[rows_a - (tap_count - 1) :], "ep", 1)
    padded = jnp.concatenate([before, glu_rows], axis=0)
    filtered = jnp.zeros(glu_rows.shape, jnp.float32)
    for offset in range(tap_count):
        filtered = filtered + conv_taps[offset] * padded[offset : offset + rows_a].astype(
            jnp.float32
        )
    sums = summed(jnp.stack([jnp.sum(filtered, axis=1), jnp.sum(filtered * filtered, axis=1)]))
    channels = conv_out_weight.shape[0]
    row_mean = sums[0] / channels
    row_square = sums[1] / channels
    scaled = (filtered - row_mean[:, None]) * lax.rsqrt(row_square - row_mean * row_mean + 1e-05)[
        :, None
    ]
    conv_hidden = jax.nn.silu(scaled * norm_gain + norm_shift).astype(jnp.bfloat16)
    return conv_hidden


def every_token(
    moe_input, moe_gain, routes, route_weights, gate, up, down, shared_gate, shared_up, shared_down
):
    rings = lax.axis_size("ep") // PAIR
    place = lax.axis_index("ep")
    side = lax.axis_index("tp") % PAIR
    rows_b = routes.shape[0]
    half = rows_b // PAIR

    def in_order(mine, other):
        return [jnp.where(side == 0, mine, other), jnp.where(side == 0, other, mine)]

    normed = norm(moe_input, moe_gain)
    down_rows = matching_rows(down)
    shared_rows = matching_rows(shared_down)
    travelling = lax.dynamic_slice_in_dim(normed, side * half, half, 0)
    arrived = []
    for back in range(rings):
        if back:
            travelling = moved(travelling, "ep", 1, 0)
        across = moved(travelling, "ep", 0, 1)
        across_rows = in_order(across, moved(across, "tp", 0, 1))
        rows = in_order(travelling, moved(travelling, "tp", 0, 1)) if back else [normed]
        arrived.append(jnp.concatenate(rows + across_rows, axis=0))
    shared_hidden = gated(normed, shared_gate, shared_up)
    total = contracted(gathered(shared_hidden), shared_rows)
    for back in range(rings):
        hidden = gated(arrived[back], gate, up)
        output = contracted(gathered(hidden), down_rows).astype(jnp.bfloat16)
        for flip in range(PAIR):
            piece = output[flip * rows_b : (flip + 1) * rows_b]
            if back or flip:
                piece = moved(piece, "ep", -back, flip)
            expert = (place // PAIR + back) % rings * PAIR + (place % PAIR ^ flip)
            weight = jnp.sum(jnp.where(routes == expert, route_weights, 0.0), axis=1, keepdims=True)
            total = total + piece.astype(jnp.float32) * weight
    return total.astype(jnp.bfloat16)


def dispatched(
    moe_input, moe_gain, routes, route_weights, gate, up, down, shared_gate, shared_up, shared_down
):
    normed = norm(moe_input, moe_gain)
    rows_b, per_row = routes.shape
    model_width = normed.shape[1]
    groups = lax.axis_size("ep")
    capacity = 2 * rows_b * per_row // groups
    flat_expert = routes.reshape(-1)
    owner_row = jnp.arange(rows_b * per_row, dtype=jnp.int32) // per_row
    expert_hits = (flat_expert[:, None] == jnp.arange(groups, dtype=jnp.int32)[None, :]).astype(
        jnp.int32
    )
    slot_rank = jnp.sum((jnp.cumsum(expert_hits, axis=0) - expert_hits) * expert_hits, axis=1)
    slot_index = flat_expert * capacity + slot_rank
    outgoing = (
        jnp.zeros((groups * capacity, model_width), jnp.bfloat16)
        .at[slot_index]
        .set(normed[owner_row])
    )
    outgoing = outgoing.reshape(groups, capacity, model_width)
    slot_share = capacity // lax.axis_size("tp")
    own_slots = lax.dynamic_slice_in_dim(outgoing, lax.axis_index("tp") * slot_share, slot_share, 1)
    partial_rows = lax.all_to_all(own_slots, "ep", split_axis=0, concat_axis=0, tiled=True)
    arrived = lax.all_gather(partial_rows, "tp", axis=1, tiled=True)
    arrived_rows = arrived.reshape(groups * capacity, model_width)
    gate_value = jnp.dot(arrived_rows, gate, preferred_element_type=jnp.float32)
    upward = jnp.dot(arrived_rows, up, preferred_element_type=jnp.float32)
    expert_hidden = (jax.nn.silu(gate_value) * upward).astype(jnp.bfloat16)
    shared_hidden = (
        jax.nn.silu(jnp.dot(normed, shared_gate, preferred_element_type=jnp.float32))
        * jnp.dot(normed, shared_up, preferred_element_type=jnp.float32)
    ).astype(jnp.bfloat16)
    columns = down.shape[1]
    routed_rows = down
    routed_sum = jnp.dot(
        lax.all_gather(expert_hidden, "tp", axis=1, tiled=True),
        routed_rows,
        preferred_element_type=jnp.float32,
    )
    shared_sum = jnp.dot(
        lax.all_gather(shared_hidden, "tp", axis=1, tiled=True),
        shared_down,
        preferred_element_type=jnp.float32,
    )
    expert_out = routed_sum.astype(jnp.bfloat16).reshape(groups, capacity, columns)
    returned = lax.all_to_all(expert_out, "ep", split_axis=0, concat_axis=0, tiled=True).reshape(
        groups * capacity, columns
    )
    picked = returned[slot_index].astype(jnp.float32) * route_weights.reshape(-1)[:, None]
    moe_sum = jnp.sum(picked.reshape(rows_b, per_row, columns), axis=1) + shared_sum
    return moe_sum.astype(jnp.bfloat16)


def body(
    conv_value,
    conv_gate,
    conv_taps,
    norm_gain,
    norm_shift,
    conv_out_weight,
    moe_input,
    moe_gain,
    routes,
    route_weights,
    expert_gate,
    expert_up,
    expert_down,
    shared_gate,
    shared_up,
    shared_down,
):
    conv_hidden = conv_module(
        conv_value, conv_gate, conv_taps, norm_gain, norm_shift, conv_out_weight
    )
    rows_b, per_row = routes.shape
    fits = 2 * rows_b * per_row // lax.axis_size("ep") < rows_b
    experts = dispatched if fits else every_token
    moe_result = experts(
        moe_input,
        moe_gain,
        routes,
        route_weights,
        expert_gate[0],
        expert_up[0],
        expert_down[0],
        shared_gate,
        shared_up,
        shared_down,
    )
    conv_result = contracted(gathered(conv_hidden), matching_rows(conv_out_weight))
    return (conv_result.astype(jnp.bfloat16), moe_result)


def solution(mesh):
    return jax.shard_map(
        body,
        mesh=mesh,
        in_specs=(
            P("ep", "tp"),
            P("ep", "tp"),
            P(None, "tp"),
            P("tp"),
            P("tp"),
            P(None, "tp"),
            P("ep", None),
            P(),
            P("ep", None),
            P("ep", None),
            P("ep", None, "tp"),
            P("ep", None, "tp"),
            P("ep", None, "tp"),
            P(None, "tp"),
            P(None, "tp"),
            P(None, "tp"),
        ),
        out_specs=(P("ep", "tp"), P("ep", "tp")),
        check_vma=False,
    )
```

```python
import jax
import jax.numpy as jnp
from jax import lax
from jax.sharding import PartitionSpec as P


PAIR = 2


def from_behind(value, axis, steps):
    count = lax.axis_size(axis)
    initial, last = (max(0, -steps), min(count, count - steps))
    return lax.ppermute(value, axis, [(source, source + steps) for source in range(initial, last)])


def moved(value, axis, steps, flip):
    count = lax.axis_size(axis)
    rings = count // PAIR
    return lax.ppermute(
        value,
        axis,
        [
            (source, ((source // PAIR + steps) % rings) * PAIR + (source % PAIR ^ flip))
            for source in range(count)
        ],
    )


def gathered(value):
    shares = [(value, moved(value, "tp", 0, 1))]
    for _ in range(lax.axis_size("tp") // PAIR - 1):
        value = moved(value, "tp", 1, 0)
        shares.append((value, moved(value, "tp", 0, 1)))
    return shares


def matching_rows(weight):
    count = lax.axis_size("tp")
    rings = count // PAIR
    index = lax.axis_index("tp")
    split = weight.reshape(count, weight.shape[0] // count, weight.shape[1])
    return [
        jnp.concatenate(
            [
                lax.dynamic_index_in_dim(
                    split, (index // PAIR + rings - back) % rings * PAIR + (index % PAIR ^ flip), 0, False
                )
                for flip in range(PAIR)
            ],
            axis=0,
        )
        for back in range(rings)
    ]


def contracted(shares, weights):
    total = None
    for pair, weight in zip(shares, weights):
        part = jnp.dot(
            jnp.concatenate(pair, axis=1), weight, preferred_element_type=jnp.float32
        )
        total = part if total is None else total + part
    return total


def summed(value):
    value = value + moved(value, "tp", 0, 1)
    total = value
    for _ in range(lax.axis_size("tp") // PAIR - 1):
        value = moved(value, "tp", 1, 0)
        total = total + value
    return total


def norm(moe_input, moe_gain):
    inputs = moe_input.astype(jnp.float32)
    return (
        inputs * lax.rsqrt(jnp.mean(inputs * inputs, axis=1, keepdims=True) + 1e-06) * moe_gain
    ).astype(jnp.bfloat16)


def gated(rows, gate, up):
    return (
        jax.nn.silu(jnp.dot(rows, gate, preferred_element_type=jnp.float32))
        * jnp.dot(rows, up, preferred_element_type=jnp.float32)
    ).astype(jnp.bfloat16)


def conv_module(conv_value, conv_gate, conv_taps, norm_gain, norm_shift, conv_out_weight):
    tap_count = conv_taps.shape[0]
    rows_a = conv_value.shape[0]
    glu_rows = (
        conv_value.astype(jnp.float32) * jax.nn.sigmoid(conv_gate.astype(jnp.float32))
    ).astype(jnp.bfloat16)
    before = from_behind(glu_rows[rows_a - (tap_count - 1) :], "ep", 1)
    padded = jnp.concatenate([before, glu_rows], axis=0)
    filtered = jnp.zeros(glu_rows.shape, jnp.float32)
    for offset in range(tap_count):
        filtered = filtered + conv_taps[offset] * padded[offset : offset + rows_a].astype(
            jnp.float32
        )
    sums = summed(jnp.stack([jnp.sum(filtered, axis=1), jnp.sum(filtered * filtered, axis=1)]))
    channels = conv_out_weight.shape[0]
    row_mean = sums[0] / channels
    row_square = sums[1] / channels
    scaled = (filtered - row_mean[:, None]) * lax.rsqrt(row_square - row_mean * row_mean + 1e-05)[
        :, None
    ]
    conv_hidden = jax.nn.silu(scaled * norm_gain + norm_shift).astype(jnp.bfloat16)
    return conv_hidden


def after(done, *values):
    held = lax.optimization_barrier((done,) + values)
    return held[0], held[1:]


def every_token(
    conv, moe_input, moe_gain, routes, route_weights, gate, up, down, shared_gate, shared_up, shared_down
):
    rings = lax.axis_size("ep") // PAIR
    place = lax.axis_index("ep")
    side = lax.axis_index("tp") % PAIR
    rows_b = routes.shape[0]
    half = rows_b // PAIR

    def in_order(value):
        other = moved(value, "tp", 0, 1)
        return [jnp.where(side == 0, value, other), jnp.where(side == 0, other, value)]

    normed = norm(moe_input, moe_gain)
    travelling = lax.dynamic_slice_in_dim(normed, side * half, half, 0)
    groups = [[(0, 0, [normed])], [(0, 1, in_order(moved(travelling, "ep", 0, 1)))]]
    for back in range(1, rings):
        travelling = moved(travelling, "ep", 1, 0)
        across = moved(travelling, "ep", 0, 1)
        groups.append([(back, 0, in_order(travelling)), (back, 1, in_order(across))])
    hidden = []
    for number, group in enumerate(groups):
        rows = jnp.concatenate([part for _, _, parts in group for part in parts], axis=0)
        value = gated(rows, gate, up)
        if number == 0:
            value, held = after(value, down, *conv)
            down, conv = held[0], held[1:]
        if number == 1:
            value, (shared_gate, shared_up, shared_down, routes, out_weight) = after(
                value, shared_gate, shared_up, shared_down, routes, conv[-1]
            )
        if number == len(groups) - 1:
            conv_hidden = conv_module(*conv)
            value, (conv_hidden,) = after(value, conv_hidden)
        hidden.append(value)
    shared_hidden = gated(normed, shared_gate, shared_up)
    total = contracted(gathered(shared_hidden), matching_rows(shared_down))
    down_rows = matching_rows(down)
    for value, group in zip(hidden, groups):
        output = contracted(gathered(value), down_rows).astype(jnp.bfloat16)
        for number, (back, flip, _) in enumerate(group):
            piece = output[number * rows_b : (number + 1) * rows_b]
            if back or flip:
                piece = moved(piece, "ep", -back, flip)
            expert = (place // PAIR + back) % rings * PAIR + (place % PAIR ^ flip)
            weight = jnp.sum(
                jnp.where(routes == expert, route_weights, 0.0), axis=1, keepdims=True
            )
            total = total + piece.astype(jnp.float32) * weight
    conv_sum = contracted(gathered(conv_hidden), matching_rows(out_weight))
    return conv_sum.astype(jnp.bfloat16), total.astype(jnp.bfloat16)


def dispatched(
    conv, moe_input, moe_gain, routes, route_weights, gate, up, down, shared_gate, shared_up, shared_down
):
    normed = norm(moe_input, moe_gain)
    rows_b, per_row = routes.shape
    model_width = normed.shape[1]
    groups = lax.axis_size("ep")
    capacity = 2 * rows_b * per_row // groups
    flat_expert = routes.reshape(-1)
    owner_row = jnp.arange(rows_b * per_row, dtype=jnp.int32) // per_row
    expert_hits = (flat_expert[:, None] == jnp.arange(groups, dtype=jnp.int32)[None, :]).astype(
        jnp.int32
    )
    slot_rank = jnp.sum((jnp.cumsum(expert_hits, axis=0) - expert_hits) * expert_hits, axis=1)
    slot_index = flat_expert * capacity + slot_rank
    outgoing = (
        jnp.zeros((groups * capacity, model_width), jnp.bfloat16)
        .at[slot_index]
        .set(normed[owner_row])
    )
    outgoing = outgoing.reshape(groups, capacity, model_width)
    slot_share = capacity // lax.axis_size("tp")
    own_slots = lax.dynamic_slice_in_dim(outgoing, lax.axis_index("tp") * slot_share, slot_share, 1)
    partial_rows = lax.all_to_all(own_slots, "ep", split_axis=0, concat_axis=0, tiled=True)
    arrived = lax.all_gather(partial_rows, "tp", axis=1, tiled=True)
    arrived_rows = arrived.reshape(groups * capacity, model_width)
    gate_value = jnp.dot(arrived_rows, gate, preferred_element_type=jnp.float32)
    upward = jnp.dot(arrived_rows, up, preferred_element_type=jnp.float32)
    expert_hidden = (jax.nn.silu(gate_value) * upward).astype(jnp.bfloat16)
    shared_hidden = (
        jax.nn.silu(jnp.dot(normed, shared_gate, preferred_element_type=jnp.float32))
        * jnp.dot(normed, shared_up, preferred_element_type=jnp.float32)
    ).astype(jnp.bfloat16)
    columns = down.shape[1]
    routed_rows = down
    routed_sum = jnp.dot(
        lax.all_gather(expert_hidden, "tp", axis=1, tiled=True),
        routed_rows,
        preferred_element_type=jnp.float32,
    )
    shared_sum = jnp.dot(
        lax.all_gather(shared_hidden, "tp", axis=1, tiled=True),
        shared_down,
        preferred_element_type=jnp.float32,
    )
    expert_out = routed_sum.astype(jnp.bfloat16).reshape(groups, capacity, columns)
    returned = lax.all_to_all(expert_out, "ep", split_axis=0, concat_axis=0, tiled=True).reshape(
        groups * capacity, columns
    )
    picked = returned[slot_index].astype(jnp.float32) * route_weights.reshape(-1)[:, None]
    moe_sum = jnp.sum(picked.reshape(rows_b, per_row, columns), axis=1) + shared_sum
    conv_sum = contracted(gathered(conv_module(*conv)), matching_rows(conv[-1]))
    return conv_sum.astype(jnp.bfloat16), moe_sum.astype(jnp.bfloat16)


def body(
    conv_value,
    conv_gate,
    conv_taps,
    norm_gain,
    norm_shift,
    conv_out_weight,
    moe_input,
    moe_gain,
    routes,
    route_weights,
    expert_gate,
    expert_up,
    expert_down,
    shared_gate,
    shared_up,
    shared_down,
):
    rows_b, per_row = routes.shape
    fits = 2 * rows_b * per_row // lax.axis_size("ep") < rows_b
    experts = dispatched if fits else every_token
    return experts(
        (conv_value, conv_gate, conv_taps, norm_gain, norm_shift, conv_out_weight),
        moe_input,
        moe_gain,
        routes,
        route_weights,
        expert_gate[0],
        expert_up[0],
        expert_down[0],
        shared_gate,
        shared_up,
        shared_down,
    )


def solution(mesh):
    return jax.shard_map(
        body,
        mesh=mesh,
        in_specs=(
            P("ep", "tp"),
            P("ep", "tp"),
            P(None, "tp"),
            P("tp"),
            P("tp"),
            P(None, "tp"),
            P("ep", None),
            P(),
            P("ep", None),
            P("ep", None),
            P("ep", None, "tp"),
            P("ep", None, "tp"),
            P("ep", None, "tp"),
            P(None, "tp"),
            P(None, "tp"),
            P(None, "tp"),
        ),
        out_specs=(P("ep", "tp"), P("ep", "tp")),
        check_vma=False,
    )
```
